32 devices in a mesh: kv: 8 (over z, y), tp: 4 (over x, core).
Axes of the slice: x: 2, y: 2, z: 4, core: 2. Of those that a mesh axis runs over, the one named last changes fastest.
Arguments:
- tokens: bfloat16 [4096, 2048], P('kv', 'tp'), may hold values from -9 to 9
- w_query: bfloat16 [2048, 1536], P(None, 'tp'), may hold values from -1 to 1
- w_key: bfloat16 [2048, 1536], P(None, 'tp'), may hold values from -1 to 1
- w_value: bfloat16 [2048, 1536], P(None, 'tp'), may hold values from -0.5 to 0.5
- w_out: bfloat16 [1536, 2048], P('tp'), may hold values from -0.15625 to 0.15625
- chosen: int32 [128, 24], P('kv'), may hold values from 0 to 127, as said below
Outputs:
- mixed: bfloat16 [4096, 2048], P(('kv', 'tp'))
The draws below stay inside these ranges and needn't reach their ends.
Inputs may be any that keep to these rules, and one draw needn't show every extreme that they name: `chosen`: row c names blocks no later than c; its first entry is c and its second c - 1 (0 for row 0), and an entry may repeat. Taking the rows in aligned runs of 16, one run for each index of kv, the rows of one run name at most 2 distinct blocks lying in any one other index's positions; in every draw some index of kv names exactly 2 from every earlier index. Every run names some block of the index just before it and of the index half the axis before it, where those exist.
All inputs are finite; a program needn't handle non-finite values.
Results may differ from the reference program's by a relative error of at most 0.014.
Values may be sent and summed in bfloat16 or wider, within the bound.
A program may use at most 320 MiB of HBM per device.

```python
import math
import jax
import jax.numpy as jnp
from jax import lax

D = 2048
HEADS = 12
HD = 128
BLK = 32
SEL = 24
MOST = 2
TOK_DEV = 512
TOKENS = 4096
N_KV = 8
N_TP = 4


def draw_tokens(key, part):
    base_key = jax.random.fold_in(key, 7)
    first, second, third = jax.random.split(base_key, 3)
    values = jnp.clip(jax.random.normal(first, (TOKENS, D), jnp.float32), -8.0, 8.0)
    return values.astype(jnp.bfloat16)


def weight_pair(key):
    first = jax.random.normal(jax.random.fold_in(key, 101), (D, HEADS * HD), jnp.float32) / math.sqrt(D)
    second = jax.random.normal(jax.random.fold_in(key, 102), (D, HEADS * HD), jnp.float32) / math.sqrt(D)
    return (first, second)


def draw_w_query(key, part):
    first, second = weight_pair(key)
    return jnp.clip(2.0 * first, -1.0, 1.0).astype(jnp.bfloat16)


def draw_w_key(key, part):
    first, second = weight_pair(key)
    values = second
    return jnp.clip(values, -1.0, 1.0).astype(jnp.bfloat16)


def draw_chosen(key, part):
    per_dev = TOK_DEV // BLK
    ndevs = N_KV
    nblocks = per_dev * ndevs
    keys = jax.random.split(jax.random.fold_in(key, 11), 7)
    popular = jnp.maximum(jax.random.randint(keys[0], (nblocks,), 0, 8) - 4, 0)
    noise = jax.random.randint(keys[1], (nblocks,), 0, 4096)
    block_ids = jnp.arange(nblocks, dtype=jnp.int32)
    score = popular * (1 << 24) + noise * 256 + block_ids % per_dev
    devices = jnp.arange(ndevs, dtype=jnp.int32)
    full_dev = jax.random.randint(keys[2], (), 1, ndevs)
    extra_full = jax.random.randint(keys[3], (ndevs,), 0, 4) == 0
    counts = jax.random.randint(keys[4], (ndevs, ndevs), 0, MOST + 1)
    is_full = (devices == full_dev) | extra_full
    counts = jnp.where(is_full[:, None], MOST, counts)
    before = devices[None, :] == devices[:, None] - 1
    halfway = devices[None, :] == devices[:, None] - ndevs // 2
    counts = jnp.where(before | halfway, jnp.maximum(counts, 1), counts)
    counts = jnp.where(devices[None, :] < devices[:, None], counts, 0)
    boost = (block_ids[None, :] == devices[:, None] * per_dev - 1).astype(jnp.int32) * (1 << 30)
    dev_score = (score[None, :] + boost).reshape(ndevs, ndevs, per_dev)
    ranks = jnp.sum((dev_score[:, :, None, :] > dev_score[:, :, :, None]).astype(jnp.int32), axis=-1)
    in_pool = (ranks < counts[:, :, None]).reshape(ndevs, nblocks)
    pool_pos = jnp.cumsum(in_pool.astype(jnp.int32), axis=1) - 1
    pool_size = jnp.sum(in_pool.astype(jnp.int32), axis=1)
    fill_slots = SEL - 2
    places = jnp.arange(fill_slots * per_dev, dtype=jnp.int32)
    hit = in_pool[:, None, :] & (pool_pos[:, None, :] == places[None, :, None])
    elements = jnp.sum(hit.astype(jnp.int32) * block_ids[None, None, :], axis=-1)
    rows_in = jnp.arange(per_dev, dtype=jnp.int32)
    slot_in = jnp.arange(fill_slots, dtype=jnp.int32)
    place_idx = slot_in[None, :] * per_dev + rows_in[:, None]
    random_pick = jax.random.randint(keys[5], (ndevs, per_dev, fill_slots), 0, 1 << 20)
    safe_size = jnp.maximum(pool_size, 1)[:, None, None]
    take = jnp.where(place_idx[None] < pool_size[:, None, None], place_idx[None], random_pick % safe_size)
    picked = jnp.take_along_axis(elements, take.reshape(ndevs, -1), axis=1).reshape(ndevs, per_dev, fill_slots)
    own_block = devices[:, None] * per_dev + rows_in[None, :]
    own_fill = devices[:, None, None] * per_dev + random_pick % (rows_in[None, :, None] + 1)
    filled = jnp.where(pool_size[:, None, None] > 0, picked, own_fill)
    prev_block = jnp.maximum(own_block - 1, 0)
    rows = jnp.concatenate([own_block[:, :, None], prev_block[:, :, None], filled], axis=-1)
    return rows.reshape(nblocks, SEL).astype(jnp.int32)


def steps_of(rng, dims, cuts, low, top_value):
    def one(axis_at, parts):
        steps = jax.random.uniform(jax.random.fold_in(jax.random.fold_in(rng, 6), axis_at), (parts,), jnp.float32, low / len(cuts), top_value / len(cuts))
        return jnp.repeat(jnp.exp(steps), dims[axis_at] // parts).reshape((-1,) + (1,) * (len(dims) - axis_at - 1))

    gain = one(*cuts[0])
    for cut in cuts[1:]:
        gain = gain * one(*cut)
    return gain


def gaussian(rng, extent, width, limit, cuts=(), kind=jnp.bfloat16):
    gain = steps_of(rng, extent, cuts, -0.22, 0.18) if cuts else 1.0
    values = jax.random.normal(rng, extent, jnp.float32) * width * gain
    return jnp.minimum(jnp.maximum(values, -limit), limit).astype(kind)


def setup_inputs(seed: int = 0) -> dict:
    key_of = jax.random.split(jax.random.key(seed), 7)
    tokens = draw_tokens(jax.random.fold_in(key_of[6], 71), 0)
    w_query = draw_w_query(jax.random.fold_in(key_of[6], 71), 0)
    w_key = draw_w_key(jax.random.fold_in(key_of[6], 71), 0)
    w_value = gaussian(key_of[3], (D, HEADS * HD), (D // 16) ** -0.5, 0.5, ((1, 4),))
    w_out = gaussian(key_of[4], (HEADS * HD, D), (HEADS * HD) ** -0.5, 0.15625, ((0, 4),))
    chosen = draw_chosen(jax.random.fold_in(key_of[6], 71), 0)
    return {"tokens": tokens, "w_query": w_query, "w_key": w_key, "w_value": w_value, "w_out": w_out, "chosen": chosen}


NEG = -1e30


def reference(tokens, w_query, w_key, w_value, w_out, chosen):
    query_rows = jnp.dot(tokens, w_query, preferred_element_type=jnp.float32).astype(jnp.bfloat16)
    key_rows = jnp.dot(tokens, w_key, preferred_element_type=jnp.float32).astype(jnp.bfloat16)
    value_rows = jnp.dot(tokens, w_value, preferred_element_type=jnp.float32).astype(jnp.bfloat16)
    total_rows = tokens.shape[0]
    block_count = total_rows // BLK
    query_blocks = query_rows.reshape(block_count, BLK, HEADS, HD)
    key_blocks = key_rows.reshape(block_count, BLK, HEADS, HD)
    value_blocks = value_rows.reshape(block_count, BLK, HEADS, HD)
    offsets = jnp.arange(BLK, dtype=jnp.int32)
    slot_ids = jnp.arange(SEL, dtype=jnp.int32)
    earlier_slot = slot_ids[None, :] < slot_ids[:, None]

    def one_block(packed):
        query_block, chosen_row, block_index = packed
        repeat_slot = jnp.any((chosen_row[:, None] == chosen_row[None, :]) & earlier_slot, axis=1)
        gathered_keys = key_blocks[chosen_row].astype(jnp.float32)
        gathered_values = value_blocks[chosen_row].astype(jnp.float32)
        scores = jnp.einsum('qhd,jkhd->hqjk', query_block.astype(jnp.float32), gathered_keys) * (HD ** -0.5)
        key_pos = chosen_row[:, None] * BLK + offsets[None, :]
        query_pos = block_index * BLK + offsets
        allowed = (~repeat_slot)[None, :, None] & (key_pos[None, :, :] <= query_pos[:, None, None])
        scores = jnp.where(allowed[None], scores, NEG)
        weights = jax.nn.softmax(scores.reshape(HEADS, BLK, SEL * BLK), axis=-1).reshape(HEADS, BLK, SEL, BLK)
        mixed_heads = jnp.einsum('hqjk,jkhd->qhd', weights, gathered_values)
        return mixed_heads.astype(jnp.bfloat16).reshape(BLK, HEADS * HD)

    attended = lax.map(one_block, (query_blocks, chosen, jnp.arange(block_count, dtype=jnp.int32)))
    attended = attended.reshape(total_rows, HEADS * HD)
    group_width = HEADS * HD // N_TP
    summed = jnp.zeros((total_rows, w_out.shape[1]), jnp.float32)
    for group in range(N_TP):
        partial_value = jnp.dot(attended[:, group * group_width:(group + 1) * group_width],
                          w_out[group * group_width:(group + 1) * group_width],
                          preferred_element_type=jnp.float32).astype(jnp.bfloat16)
        partial_value = lax.optimization_barrier(partial_value)
        summed = summed + partial_value.astype(jnp.float32)
    return summed.astype(jnp.bfloat16)
```

```python
import functools

import jax
import jax.numpy as jnp
from jax import lax
from jax.experimental import pallas as pl
from jax.experimental.pallas import tpu as pltpu
from jax.sharding import PartitionSpec as P

HD = 128
BLK = 32
MOST = 2
NEG = -1e30
BF = jnp.bfloat16
F32 = jnp.float32
MESH = pl.DeviceIdType.MESH
OWN_CHUNKS = 4
OUT_CHUNKS = 4


def dot(a, b):
    return jnp.dot(a, b, preferred_element_type=F32)


def dot_nt(a, b):
    return lax.dot_general(a, b, (((1,), (1,)), ((), ())), preferred_element_type=F32)


def iota(shape, dim):
    return lax.broadcasted_iota(jnp.int32, shape, dim)


def kernel(
    n, tok, wq, wk, wv, wo, chosen, out,
    wbuf, wobuf, gat, far, pick, ask, asked, acc, accf, qb, kb, vb, kf, vf,
    bias, biasf, top, tot, summed, att, hold, psend, precv, xsend, xrecv, mine,
    wsem, ox_s, ox_r, oc_s, oc_r, of_s, of_r, rq_s, rq_r, fk_s, fk_r,
    fx_s, fx_r, fc_s, fc_r, ff_s, ff_r, pd_s, pd_r, px_s, px_r,
):
    rows, feat = tok.shape
    width = wq.shape[1]
    heads = width // HD
    per = rows // BLK
    blocks = n * per
    slot = MOST * BLK
    cols = wo.shape[1]
    quarter = rows // 4
    me = lax.axis_index("kv")
    t = lax.axis_index("tp")
    mate = t + 1 - 2 * lax.rem(t, 2)
    across = lax.rem(t + 2, 4)
    diag = lax.rem(mate + 2, 4)
    order = (t, mate, across, diag)

    loads = []
    for d in range(4):
        for j, w in enumerate((wq, wk, wv)):
            src = pl.ds(pl.multiple_of(order[d] * feat, feat), feat)
            c = pltpu.make_async_copy(w.at[src, :], wbuf.at[j, d], wsem.at[d * 3 + j])
            c.start()
            loads.append(c)
    wo_load = pltpu.make_async_copy(wo, wobuf, wsem.at[12])
    wo_load.start()

    barrier = pltpu.get_barrier_semaphore()
    for d in range(1, 4):
        pl.semaphore_signal(barrier, inc=1, device_id=(me, order[d]), device_id_type=MESH)
    for k in range(1, n):
        pl.semaphore_signal(
            barrier, inc=1, device_id=(lax.rem(me + k, n), t), device_id_type=MESH
        )
    pl.semaphore_wait(barrier, n + 2)

    def remote(src, dst, s, r, who):
        c = pltpu.make_async_remote_copy(
            src_ref=src, dst_ref=dst, send_sem=s, recv_sem=r, device_id=who, device_id_type=MESH
        )
        return c

    piece = rows // OWN_CHUNKS
    own_x = []
    for c in range(OWN_CHUNKS):
        part = pl.ds(c * piece, piece)
        own_x.append(
            remote(tok.at[part], gat.at[1, part], ox_s.at[c], ox_r.at[c], (me, across))
        )
        own_x[-1].start()
    own_c = remote(tok, gat.at[0], oc_s, oc_r, (me, mate))
    own_c.start()

    lane = iota((per, blocks), 1)
    seen = jnp.zeros((per, blocks), jnp.int32)
    picks = chosen[...]
    for j in range(picks.shape[1]):
        seen = jnp.maximum(seen, (picks[:, j : j + 1] == lane).astype(jnp.int32))
    wanted = jnp.max(seen, axis=0, keepdims=True)
    lane1 = iota((1, blocks), 1)
    inside = (lane1 >= me * per) & (lane1 < me * per + per)
    wanted = jnp.where(inside, 0, wanted)
    ask[...] = jnp.broadcast_to(wanted, (8, blocks))
    asks = []
    for k in range(1, n):
        c = remote(
            ask, asked.at[k - 1], rq_s.at[k - 1], rq_r.at[k - 1], (lax.rem(me + n - k, n), t)
        )
        c.start()
        asks.append(c)

    ia, ib = iota((blocks, blocks), 0), iota((blocks, blocks), 1)
    tri = ((lax.div(ia, per) == lax.div(ib, per)) & (ia <= ib)).astype(BF)
    seen_b = seen.astype(F32).astype(BF)
    want8 = jnp.broadcast_to(wanted, (8, blocks)).astype(F32)
    rank8 = dot(want8.astype(BF), tri) * want8
    rank = rank8[0:1, :]
    spots = n * slot
    col = iota((spots, blocks), 0)
    blk = iota((spots, blocks), 1)
    away = me - lax.div(blk, per)
    away = jnp.where(away < 0, away + n, away)
    hit = (lax.div(col, slot) == away - 1) & (
        jnp.broadcast_to(rank, (spots, blocks))
        == (lax.div(lax.rem(col, slot), BLK) + 1).astype(F32)
    )
    hit = hit.astype(F32).astype(BF)
    far_seen = dot_nt(seen_b, hit)
    grow = (lax.div(iota((rows, per), 0), BLK) == iota((rows, per), 1)).astype(F32).astype(BF)
    biasf[...] = jnp.where(dot(grow, far_seen.astype(BF)) > 0.5, 0.0, NEG)
    spread = (
        (iota((blocks, rows), 0) == me * per + lax.div(iota((blocks, rows), 1), BLK))
        .astype(F32)
        .astype(BF)
    )
    own_seen = dot(grow, dot(seen_b, spread).astype(BF))
    causal = iota((rows, rows), 1) <= iota((rows, rows), 0)
    bias[...] = jnp.where((own_seen > 0.5) & causal, 0.0, NEG)

    for c in asks:
        c.wait_recv()
    others = asked[:, 0, :].astype(F32)
    ranks = dot(others.astype(BF), tri) * others
    places = dot(ranks.astype(BF), spread)
    srow, scol = iota((slot, rows), 0), iota((slot, rows), 1)
    same = lax.rem(srow, BLK) == lax.rem(scol, BLK)
    want_rank = (lax.div(srow, BLK) + 1).astype(F32)
    sends = []
    for k in range(1, n):
        sel = same & (jnp.broadcast_to(places[k - 1 : k, :], (slot, rows)) == want_rank)
        pick[k - 1] = dot(sel.astype(F32).astype(BF), tok[...]).astype(BF)
        c = remote(
            pick.at[k - 1],
            far.at[0, pl.ds((k - 1) * slot, slot)],
            fk_s.at[k - 1],
            fk_r.at[k - 1],
            (lax.rem(me + k, n), t),
        )
        c.start()
        sends.append(c)

    half = rows // 2

    def project(d, src, first):
        for c in loads[3 * d : 3 * d + 3]:
            c.wait()
        for j in range(3):
            for r in range(2):
                part = pl.ds(r * half, half)
                val = dot(src[part, :], wbuf[j, d])
                if first:
                    acc[j, part, :] = val
                else:
                    acc[j, part, :] += val

    project(0, tok, True)
    own_c.wait_recv()
    project(1, gat.at[0], False)

    fwd = []
    for c in range(OWN_CHUNKS):
        own_x[c].wait_recv()
        part = pl.ds(c * piece, piece)
        f = remote(gat.at[1, part], gat.at[2, part], of_s.at[c], of_r.at[c], (me, mate))
        f.start()
        fwd.append(f)

    far_x, far_c = [], []
    for k in range(1, n):
        part = pl.ds((k - 1) * slot, slot)
        sends[k - 1].wait_recv()
        c = remote(far.at[0, part], far.at[2, part], fx_s.at[k - 1], fx_r.at[k - 1], (me, across))
        c.start()
        far_x.append(c)
        c = remote(far.at[0, part], far.at[1, part], fc_s.at[k - 1], fc_r.at[k - 1], (me, mate))
        c.start()
        far_c.append(c)

    project(2, gat.at[1], False)
    for f in fwd:
        f.wait_recv()
    project(3, gat.at[2], False)
    qb[...] = acc[0].astype(BF)
    kb[...] = acc[1].astype(BF)
    vb[...] = acc[2].astype(BF)

    scale = HD ** (-0.5)
    step = rows // 4
    for h in range(heads):
        hc = slice(h * HD, (h + 1) * HD)
        for r in range(4):
            rr = slice(r * step, (r + 1) * step)
            upto = (r + 1) * step
            s = dot_nt(qb[rr, hc], kb[:upto, hc]) * scale + bias[rr, :upto]
            m = jnp.max(s, axis=1, keepdims=True)
            p = jnp.exp(s - m)
            top[h, rr, :] = m
            tot[h, rr, :] = jnp.sum(p, axis=1, keepdims=True)
            summed[h, rr, :] = dot(p.astype(BF), vb[:upto, hc])

    far_f = []
    for k in range(1, n):
        part = pl.ds((k - 1) * slot, slot)
        far_x[k - 1].wait_recv()
        f = remote(far.at[2, part], far.at[3, part], ff_s.at[k - 1], ff_r.at[k - 1], (me, mate))
        f.start()
        far_f.append(f)
    used = (n - 1) * slot
    for c in far_c:
        c.wait_recv()
    for d in range(3):
        for j in range(2):
            val = dot(far[d], wbuf[1 + j, d])
            if d == 0:
                accf[j] = val
            else:
                accf[j] += val
    for c in far_f:
        c.wait_recv()
    for j, dst in enumerate((kf, vf)):
        dst[pl.ds(0, used), :] = (accf[j] + dot(far[3], wbuf[1 + j, 3])).astype(BF)
        dst[pl.ds(used, spots - used), :] = jnp.zeros((spots - used, width), BF)

    def finish(who):
        part = pl.ds(pl.multiple_of(who * quarter, quarter), quarter)
        for h in range(heads):
            hc = slice(h * HD, (h + 1) * HD)
            s = dot_nt(qb[part, hc], kf[:, hc]) * scale + biasf[part, :]
            m0 = top[h, part, :]
            m = jnp.maximum(m0, jnp.max(s, axis=1, keepdims=True))
            p = jnp.exp(s - m)
            keep = jnp.exp(m0 - m)
            total = tot[h, part, :] * keep + jnp.sum(p, axis=1, keepdims=True)
            val = summed[h, part, :] * keep + dot(p.astype(BF), vf[:, hc])
            att[part, hc] = (val / total).astype(BF)
        return part

    wo_load.wait()
    wide = cols // OUT_CHUNKS
    to_mate, to_across = [], []

    def share(which, who):
        part = finish(who)
        for c in range(OUT_CHUNKS):
            psend[which, c] = dot(att[part, :], wobuf[:, c * wide : (c + 1) * wide]).astype(BF)
            i = which * OUT_CHUNKS + c
            x = remote(
                psend.at[which, c], precv.at[which, c], pd_s.at[i], pd_r.at[i], (me, mate)
            )
            x.start()
            to_mate.append(x)

    share(0, diag)
    part = finish(across)
    for c in range(OUT_CHUNKS):
        val = dot(att[part, :], wobuf[:, c * wide : (c + 1) * wide])
        to_mate[c].wait_recv()
        xsend[c] = (val + precv[0, c].astype(F32)).astype(BF)
        x = remote(xsend.at[c], xrecv.at[c], px_s.at[c], px_r.at[c], (me, across))
        x.start()
        to_across.append(x)
    share(1, mate)
    part = finish(t)
    for c in range(OUT_CHUNKS):
        val = dot(att[part, :], wobuf[:, c * wide : (c + 1) * wide])
        to_mate[OUT_CHUNKS + c].wait_recv()
        mine[c] = val + precv[1, c].astype(F32)
    for c in range(OUT_CHUNKS):
        to_across[c].wait_recv()
        out[:, c * wide : (c + 1) * wide] = (mine[c] + xrecv[c].astype(F32)).astype(BF)

    for c in own_x + [own_c] + asks + sends + fwd + far_x + far_c + far_f + to_mate + to_across:
        c.wait_send()


def local(n, tokens, w_query, w_key, w_value, w_out, chosen):
    rows, feat = tokens.shape
    width = w_query.shape[1]
    heads = width // HD
    cols = w_out.shape[1]
    blocks = n * (rows // BLK)
    slot = MOST * BLK
    used, spots = (n - 1) * slot, n * slot
    quarter = rows // 4
    wide = cols // OUT_CHUNKS
    vmem = pl.BlockSpec(memory_space=pltpu.VMEM)
    hbm = pl.BlockSpec(memory_space=pl.ANY)
    dma = pltpu.SemaphoreType.DMA
    V = pltpu.VMEM
    return pl.pallas_call(
        functools.partial(kernel, n),
        out_shape=jax.ShapeDtypeStruct((quarter, cols), BF),
        in_specs=[vmem, hbm, hbm, hbm, hbm, vmem],
        out_specs=vmem,
        scratch_shapes=[
            V((3, 4, feat, width), BF),
            V((width, cols), BF),
            V((3, rows, feat), BF),
            V((4, used, feat), BF),
            V((n - 1, slot, feat), BF),
            V((8, blocks), jnp.int32),
            V((n - 1, 8, blocks), jnp.int32),
            V((3, rows, width), F32),
            V((2, used, width), F32),
            V((rows, width), BF),
            V((rows, width), BF),
            V((rows, width), BF),
            V((spots, width), BF),
            V((spots, width), BF),
            V((rows, rows), F32),
            V((rows, spots), F32),
            V((heads, rows, 1), F32),
            V((heads, rows, 1), F32),
            V((heads, rows, HD), F32),
            V((rows, width), BF),
            V((8, 128), F32),
            V((2, OUT_CHUNKS, quarter, wide), BF),
            V((2, OUT_CHUNKS, quarter, wide), BF),
            V((OUT_CHUNKS, quarter, wide), BF),
            V((OUT_CHUNKS, quarter, wide), BF),
            V((OUT_CHUNKS, quarter, wide), F32),
            dma((13,)),
            dma((OWN_CHUNKS,)), dma((OWN_CHUNKS,)),
            dma, dma,
            dma((OWN_CHUNKS,)), dma((OWN_CHUNKS,)),
            dma((n - 1,)), dma((n - 1,)),
            dma((n - 1,)), dma((n - 1,)),
            dma((n - 1,)), dma((n - 1,)),
            dma((n - 1,)), dma((n - 1,)),
            dma((n - 1,)), dma((n - 1,)),
            dma((2 * OUT_CHUNKS,)), dma((2 * OUT_CHUNKS,)),
            dma((OUT_CHUNKS,)), dma((OUT_CHUNKS,)),
        ],
        compiler_params=pltpu.CompilerParams(
            collective_id=0, has_side_effects=True, vmem_limit_bytes=60 * 1024 * 1024
        ),
    )(tokens, w_query, w_key, w_value, w_out, chosen)


def solution(mesh):
    return jax.shard_map(
        functools.partial(local, mesh.shape["kv"]),
        mesh=mesh,
        in_specs=(
            P("kv", "tp"),
            P(None, "tp"),
            P(None, "tp"),
            P(None, "tp"),
            P("tp", None),
            P("kv", None),
        ),
        out_specs=P(("kv", "tp"), None),
        check_vma=False,
    )
```

```python
import functools

import jax
import jax.numpy as jnp
from jax import lax
from jax.experimental import pallas as pl
from jax.experimental.pallas import tpu as pltpu
from jax.sharding import PartitionSpec as P

HD = 128
BLK = 32
MOST = 2
NEG = -1e30
LOG2E = 1.4426950408889634
BF = jnp.bfloat16
F32 = jnp.float32
MESH = pl.DeviceIdType.MESH
OWN_CHUNKS = 4
OUT_CHUNKS = 4


def dot(a, b):
    return jnp.dot(a, b, preferred_element_type=F32)


def dot_nt(a, b):
    return lax.dot_general(a, b, (((1,), (1,)), ((), ())), preferred_element_type=F32)


def quot(x, size):
    if size & (size - 1) == 0:
        return lax.shift_right_logical(x, jnp.full(x.shape, size.bit_length() - 1, x.dtype))
    return lax.div(x, size)


def rest(x, size):
    if size & (size - 1) == 0:
        return x & (size - 1)
    return lax.rem(x, size)


def iota(shape, dim):
    return lax.broadcasted_iota(jnp.int32, shape, dim)


def kernel(
    n, tok, wq, wk, wv, wo, chosen, out,
    wbuf, wobuf, gat, far, pick, ask, asked, acc, accf, qb, kb, vb, kf, vf,
    bias, biasf, top, tot, summed, att, psend, precv, xsend, xrecv, mine,
    wsem, ox_s, ox_r, oc_s, oc_r, of_s, of_r, rq_s, rq_r, fk_s, fk_r,
    fx_s, fx_r, fc_s, fc_r, ff_s, ff_r, pd_s, pd_r, px_s, px_r,
):
    rows, feat = tok.shape
    width = wq.shape[1]
    heads = width // HD
    per = rows // BLK
    blocks = n * per
    slot = MOST * BLK
    cols = wo.shape[1]
    quarter = rows // 4
    me = lax.axis_index("kv")
    t = lax.axis_index("tp")
    mate = t + 1 - 2 * lax.rem(t, 2)
    across = lax.rem(t + 2, 4)
    diag = lax.rem(mate + 2, 4)
    order = (t, mate, across, diag)

    loads = []
    for d in range(4):
        for j, w in enumerate((wq, wk, wv)):
            src = pl.ds(pl.multiple_of(order[d] * feat, feat), feat)
            c = pltpu.make_async_copy(w.at[src, :], wbuf.at[j, d], wsem.at[d * 3 + j])
            c.start()
            loads.append(c)
    wo_load = pltpu.make_async_copy(wo, wobuf, wsem.at[12])
    wo_load.start()

    barrier = pltpu.get_barrier_semaphore()
    for d in range(1, 4):
        pl.semaphore_signal(barrier, inc=1, device_id=(me, order[d]), device_id_type=MESH)
    for k in range(1, n):
        pl.semaphore_signal(
            barrier, inc=1, device_id=(lax.rem(me + k, n), t), device_id_type=MESH
        )
    pl.semaphore_wait(barrier, n + 2)

    def remote(src, dst, s, r, who):
        c = pltpu.make_async_remote_copy(
            src_ref=src, dst_ref=dst, send_sem=s, recv_sem=r, device_id=who, device_id_type=MESH
        )
        return c

    piece = rows // OWN_CHUNKS
    own_x = []
    for c in range(OWN_CHUNKS):
        part = pl.ds(c * piece, piece)
        own_x.append(
            remote(tok.at[part], gat.at[1, part], ox_s.at[c], ox_r.at[c], (me, across))
        )
        own_x[-1].start()
    own_c = remote(tok, gat.at[0], oc_s, oc_r, (me, mate))
    own_c.start()

    lane = iota((per, blocks), 1)
    seen = jnp.zeros((per, blocks), jnp.int32)
    picks = chosen[...]
    for j in range(picks.shape[1]):
        seen = jnp.maximum(seen, (picks[:, j : j + 1] == lane).astype(jnp.int32))
    wanted = jnp.max(seen, axis=0, keepdims=True)
    lane1 = iota((1, blocks), 1)
    inside = (lane1 >= me * per) & (lane1 < me * per + per)
    wanted = jnp.where(inside, 0, wanted)
    ask[...] = jnp.broadcast_to(wanted, (8, blocks))
    asks = []
    for k in range(1, n):
        c = remote(
            ask, asked.at[k - 1], rq_s.at[k - 1], rq_r.at[k - 1], (lax.rem(me + n - k, n), t)
        )
        c.start()
        asks.append(c)

    ia, ib = iota((blocks, blocks), 0), iota((blocks, blocks), 1)
    tri = ((quot(ia, per) == quot(ib, per)) & (ia <= ib)).astype(BF)
    seen_b = seen.astype(F32).astype(BF)
    want8 = jnp.broadcast_to(wanted, (8, blocks)).astype(F32)
    rank8 = dot(want8.astype(BF), tri) * want8
    rank = rank8[0:1, :]
    spread = (
        (iota((blocks, rows), 0) == me * per + quot(iota((blocks, rows), 1), BLK))
        .astype(F32)
        .astype(BF)
    )
    for c in asks:
        c.wait_recv()
    others = asked[:, 0, :].astype(F32)
    ranks = dot(others.astype(BF), tri) * others
    places = dot(ranks.astype(BF), spread)
    srow, scol = iota((slot, rows), 0), iota((slot, rows), 1)
    same = rest(srow, BLK) == rest(scol, BLK)
    want_rank = (quot(srow, BLK) + 1).astype(F32)
    sends = []
    for k in range(1, n):
        sel = same & (jnp.broadcast_to(places[k - 1 : k, :], (slot, rows)) == want_rank)
        pick[k - 1] = dot(sel.astype(F32).astype(BF), tok[...]).astype(BF)
        c = remote(
            pick.at[k - 1],
            far.at[0, pl.ds((k - 1) * slot, slot)],
            fk_s.at[k - 1],
            fk_r.at[k - 1],
            (lax.rem(me + k, n), t),
        )
        c.start()
        sends.append(c)

    half = rows // 2

    def project(d, src, first):
        for c in loads[3 * d : 3 * d + 3]:
            c.wait()
        for j in range(3):
            for r in range(2):
                part = pl.ds(r * half, half)
                val = dot(src[part, :], wbuf[j, d])
                if first:
                    acc[j, part, :] = val
                else:
                    acc[j, part, :] += val

    project(0, tok, True)
    spots = n * slot
    col = iota((spots, blocks), 0)
    blk = iota((spots, blocks), 1)
    away = me - quot(blk, per)
    away = jnp.where(away < 0, away + n, away)
    hit = (quot(col, slot) == away - 1) & (
        jnp.broadcast_to(rank, (spots, blocks))
        == (quot(rest(col, slot), BLK) + 1).astype(F32)
    )
    hit = hit.astype(F32).astype(BF)
    far_seen = dot_nt(seen_b, hit)
    grow = (quot(iota((rows, per), 0), BLK) == iota((rows, per), 1)).astype(F32).astype(BF)
    biasf[...] = jnp.where(dot(grow, far_seen.astype(BF)) > 0.5, 0.0, NEG)
    own_seen = dot(grow, dot(seen_b, spread).astype(BF))
    causal = iota((rows, rows), 1) <= iota((rows, rows), 0)
    bias[...] = jnp.where((own_seen > 0.5) & causal, 0.0, NEG)


    own_c.wait_recv()
    project(1, gat.at[0], False)

    fwd, far_x, far_c = [], [], []

    def hand_own(c):
        own_x[c].wait_recv()
        part = pl.ds(c * piece, piece)
        f = remote(gat.at[1, part], gat.at[2, part], of_s.at[c], of_r.at[c], (me, mate))
        f.start()
        fwd.append(f)

    def hand_far(k):
        part = pl.ds((k - 1) * slot, slot)
        sends[k - 1].wait_recv()
        c = remote(far.at[0, part], far.at[2, part], fx_s.at[k - 1], fx_r.at[k - 1], (me, across))
        c.start()
        far_x.append(c)
        c = remote(far.at[0, part], far.at[1, part], fc_s.at[k - 1], fc_r.at[k - 1], (me, mate))
        c.start()
        far_c.append(c)

    for k in range(1, n):
        hand_far(k)
        at = k * OWN_CHUNKS // (n - 1)
        for c in range((k - 1) * OWN_CHUNKS // (n - 1), at):
            hand_own(c)

    project(2, gat.at[1], False)
    for f in fwd:
        f.wait_recv()
    project(3, gat.at[2], False)
    qb[...] = acc[0].astype(BF)
    kb[...] = acc[1].astype(BF)
    vb[...] = acc[2].astype(BF)

    scale = HD ** (-0.5) * LOG2E
    step = rows // 4
    cut = [slice(h * HD, (h + 1) * HD) for h in range(heads)]
    for r in range(4):
        rr = slice(r * step, (r + 1) * step)
        upto = (r + 1) * step
        shade = bias[rr, :upto]
        ss = [dot_nt(qb[rr, hc], kb[:upto, hc]) * scale + shade for hc in cut]
        ms = [jnp.max(x, axis=1, keepdims=True) for x in ss]
        ps = [jnp.exp2(x - m) for x, m in zip(ss, ms)]
        vals = [dot(p.astype(BF), vb[:upto, hc]) for p, hc in zip(ps, cut)]
        for h in range(heads):
            top[h, rr, :] = ms[h]
            tot[h, rr, :] = jnp.sum(ps[h], axis=1, keepdims=True)
            summed[h, rr, :] = vals[h]

    def project_far(d):
        for j in range(2):
            val = dot(far[d], wbuf[1 + j, d])
            if d == 0:
                accf[j] = val
            else:
                accf[j] += val

    project_far(0)
    for c in far_c:
        c.wait_recv()
    project_far(1)
    far_f = []
    used = (n - 1) * slot
    for k in range(1, n):
        part = pl.ds((k - 1) * slot, slot)
        far_x[k - 1].wait_recv()
        f = remote(far.at[2, part], far.at[3, part], ff_s.at[k - 1], ff_r.at[k - 1], (me, mate))
        f.start()
        far_f.append(f)
    project_far(2)
    for c in far_f:
        c.wait_recv()
    for j, dst in enumerate((kf, vf)):
        dst[pl.ds(0, used), :] = (accf[j] + dot(far[3], wbuf[1 + j, 3])).astype(BF)
        dst[pl.ds(used, spots - used), :] = jnp.zeros((spots - used, width), BF)

    def finish(who):
        part = pl.ds(pl.multiple_of(who * quarter, quarter), quarter)
        shade = biasf[part, :]
        ss = [dot_nt(qb[part, hc], kf[:, hc]) * scale + shade for hc in cut]
        old = [top[h, part, :] for h in range(heads)]
        ms = [jnp.maximum(m, jnp.max(x, axis=1, keepdims=True)) for m, x in zip(old, ss)]
        ps = [jnp.exp2(x - m) for x, m in zip(ss, ms)]
        keep = [jnp.exp2(m0 - m) for m0, m in zip(old, ms)]
        vals = [dot(p.astype(BF), vf[:, hc]) for p, hc in zip(ps, cut)]
        for h in range(heads):
            total = tot[h, part, :] * keep[h] + jnp.sum(ps[h], axis=1, keepdims=True)
            val = summed[h, part, :] * keep[h] + vals[h]
            att[part, cut[h]] = (val / total).astype(BF)
        return part

    wo_load.wait()
    wide = cols // OUT_CHUNKS
    to_mate, to_across = [], []

    def share(which, who):
        part = finish(who)
        for c in range(OUT_CHUNKS):
            psend[which, c] = dot(att[part, :], wobuf[:, c * wide : (c + 1) * wide]).astype(BF)
            i = which * OUT_CHUNKS + c
            x = remote(
                psend.at[which, c], precv.at[which, c], pd_s.at[i], pd_r.at[i], (me, mate)
            )
            x.start()
            to_mate.append(x)

    share(0, diag)
    part = finish(across)
    for c in range(OUT_CHUNKS):
        val = dot(att[part, :], wobuf[:, c * wide : (c + 1) * wide])
        to_mate[c].wait_recv()
        xsend[c] = (val + precv[0, c].astype(F32)).astype(BF)
        x = remote(xsend.at[c], xrecv.at[c], px_s.at[c], px_r.at[c], (me, across))
        x.start()
        to_across.append(x)
    share(1, mate)
    part = finish(t)
    for c in range(OUT_CHUNKS):
        val = dot(att[part, :], wobuf[:, c * wide : (c + 1) * wide])
        to_mate[OUT_CHUNKS + c].wait_recv()
        mine[c] = val + precv[1, c].astype(F32)
    for c in range(OUT_CHUNKS):
        to_across[c].wait_recv()
        out[:, c * wide : (c + 1) * wide] = (mine[c] + xrecv[c].astype(F32)).astype(BF)

    for c in own_x + [own_c] + asks + sends + fwd + far_x + far_c + far_f + to_mate + to_across:
        c.wait_send()


def local(n, tokens, w_query, w_key, w_value, w_out, chosen):
    rows, feat = tokens.shape
    width = w_query.shape[1]
    heads = width // HD
    cols = w_out.shape[1]
    blocks = n * (rows // BLK)
    slot = MOST * BLK
    used, spots = (n - 1) * slot, n * slot
    quarter = rows // 4
    wide = cols // OUT_CHUNKS
    vmem = pl.BlockSpec(memory_space=pltpu.VMEM)
    hbm = pl.BlockSpec(memory_space=pltpu.HBM)
    dma = pltpu.SemaphoreType.DMA
    V = pltpu.VMEM
    return pl.pallas_call(
        functools.partial(kernel, n),
        out_shape=jax.ShapeDtypeStruct((quarter, cols), BF),
        in_specs=[vmem, hbm, hbm, hbm, hbm, vmem],
        out_specs=vmem,
        scratch_shapes=[
            V((3, 4, feat, width), BF),
            V((width, cols), BF),
            V((3, rows, feat), BF),
            V((4, used, feat), BF),
            V((n - 1, slot, feat), BF),
            V((8, blocks), jnp.int32),
            V((n - 1, 8, blocks), jnp.int32),
            V((3, rows, width), F32),
            V((2, used, width), F32),
            V((rows, width), BF),
            V((rows, width), BF),
            V((rows, width), BF),
            V((spots, width), BF),
            V((spots, width), BF),
            V((rows, rows), F32),
            V((rows, spots), F32),
            V((heads, rows, 1), F32),
            V((heads, rows, 1), F32),
            V((heads, rows, HD), F32),
            V((rows, width), BF),
            V((2, OUT_CHUNKS, quarter, wide), BF),
            V((2, OUT_CHUNKS, quarter, wide), BF),
            V((OUT_CHUNKS, quarter, wide), BF),
            V((OUT_CHUNKS, quarter, wide), BF),
            V((OUT_CHUNKS, quarter, wide), F32),
            dma((13,)),
            dma((OWN_CHUNKS,)), dma((OWN_CHUNKS,)),
            dma, dma,
            dma((OWN_CHUNKS,)), dma((OWN_CHUNKS,)),
            dma((n - 1,)), dma((n - 1,)),
            dma((n - 1,)), dma((n - 1,)),
            dma((n - 1,)), dma((n - 1,)),
            dma((n - 1,)), dma((n - 1,)),
            dma((n - 1,)), dma((n - 1,)),
            dma((2 * OUT_CHUNKS,)), dma((2 * OUT_CHUNKS,)),
            dma((OUT_CHUNKS,)), dma((OUT_CHUNKS,)),
        ],
        compiler_params=pltpu.CompilerParams(
            collective_id=0, has_side_effects=True, vmem_limit_bytes=60 * 1024 * 1024
        ),
    )(tokens, w_query, w_key, w_value, w_out, chosen)


def solution(mesh):
    return jax.shard_map(
        functools.partial(local, mesh.shape["kv"]),
        mesh=mesh,
        in_specs=(
            P("kv", "tp"),
            P(None, "tp"),
            P(None, "tp"),
            P(None, "tp"),
            P("tp", None),
            P("kv", None),
        ),
        out_specs=P(("kv", "tp"), None),
        check_vma=False,
    )
```
